32 devices in a mesh: sp: 8 (over z, y), tp: 4 (over x, core).
Axes of the slice: x: 2, y: 2, z: 4, core: 2. Of those that a mesh axis runs over, the one named last changes fastest.
Arguments:
- arriving_hidden_sum: bfloat16 [8192, 2048], P('sp'), may hold values from -40 to 40
- content_entries_clustered: bfloat16 [8192, 4096], P('sp', 'tp'), may hold values from -6 to 6
- leaving_switch_entries: bfloat16 [8192, 4096], P('sp', 'tp'), may hold values from -6 to 6
- linked_source_target_pairs: bfloat16 [8192, 8, 2, 128], P('sp', 'tp'), may hold values from -1.78125 to 1.78125
- raw_interval_length: bfloat16 [8192, 64], P('sp', 'tp'), may hold values from -5 to 5
- spike_extra_lognoise: float32 [8192, 64], P('sp', 'tp'), may hold values from -0.6 to 0
- content_filter_kernel: bfloat16 [4, 4096], P(None, 'tp'), may hold values from -3 to 3
- coupling_filter_kernel: bfloat16 [4, 8, 2, 128], P(None, 'tp'), may hold values from -3 to 3
- interval_shift_vector: float32 [64], P('tp'), may hold values from -0.5 to 0.5
- fading_speed_exponent: float32 [64], P('tp'), may hold values from -16 to -2.9
- skip_channel_factor: float32 [64], P('tp'), may hold values from 1 to 10
- cluster_rescale_vector: float32 [4096], P('tp'), may hold values from 0.1 to 1.9
- blender_final_tensor: bfloat16 [4096, 2048], P('tp'), may hold values from -0.09375 to 0.09375
- prelayer_rescale_vector: float32 [2048], replicated, may hold values from 0.1 to 1.9
- switching_linear_tensor: bfloat16 [2048, 5632], P('sp', 'tp'), may hold values from -0.125 to 0.125
- widening_linear_tensor: bfloat16 [2048, 5632], P('sp', 'tp'), may hold values from -0.125 to 0.125
- contracting_linear_tensor: bfloat16 [5632, 2048], P('tp', 'sp'), may hold values from -0.078125 to 0.078125
Outputs:
- residual_out: bfloat16 [8192, 2048], P('sp', 'tp')
The draws below stay inside these ranges and needn't reach their ends.
All inputs are finite; a program needn't handle non-finite values.
Results may differ from the reference program's by a relative error of at most 0.012.
Values may be sent and summed in bfloat16 or wider, within the bound.
A program may use at most 128 MiB of HBM per device.

```python
import math
import jax
import jax.numpy as jnp
from jax import lax

D = 2048
HEADS = 64
HEAD_DIM = 64
GROUPS = 8
STATE = 128
FF = 5632
CONV = 4
BLOCK_POSITIONS = 128
TOK_DEV = 1024
DI = 4096
TOKENS = 8192
N_TP = 4


def draw_arriving_hidden_sum(key, part):
    noise_key = jax.random.fold_in(key, 11)
    col_key = jax.random.fold_in(key, 12)
    row_key = jax.random.fold_in(key, 13)
    columns = jnp.arange(D, dtype=jnp.float32) / D
    row_scale = jnp.exp(jax.random.uniform(row_key, (TOKENS, 1), jnp.float32, jnp.log(0.4), jnp.log(4.0)))
    base = jnp.clip(jax.random.normal(noise_key, (TOKENS, D), jnp.float32), -6.0, 6.0)
    col_scale = 12.0 ** columns * jnp.exp(jax.random.uniform(col_key, (D,), jnp.float32, -0.35, 0.35))
    return jnp.clip(0.2 * base * row_scale * col_scale, -40.0, 40.0).astype(jnp.bfloat16)


def draw_raw_interval_length(key, part):
    noise_key = jax.random.fold_in(key, 21)
    shift_key = jax.random.fold_in(key, 22)
    shifts = jax.random.uniform(shift_key, (TOKENS // TOK_DEV, 1, 1), jnp.float32, -1.0, 1.0)
    noise = jnp.clip(0.7 * jax.random.normal(noise_key, (TOKENS // TOK_DEV, TOK_DEV, HEADS), jnp.float32), -4.0, 4.0)
    return (noise + shifts).reshape(TOKENS, HEADS).astype(jnp.bfloat16)


def draw_spike_extra_lognoise(key, part):
    spot_key = jax.random.fold_in(key, 31)
    loss_key = jax.random.fold_in(key, 32)
    spots = jax.random.randint(spot_key, (3,), 0, TOKENS)
    losses = jnp.log(jax.random.uniform(loss_key, (3, HEADS), jnp.float32, 0.55, 0.8))
    return jnp.zeros((TOKENS, HEADS), jnp.float32).at[spots].add(losses)


def draw_fading_speed_exponent(key, part):
    pick_key = jax.random.fold_in(key, 41)
    fast_key = jax.random.fold_in(key, 42)
    slow_key = jax.random.fold_in(key, 43)
    share = 0.5
    fast_pick = jax.random.uniform(pick_key, (HEADS,), jnp.float32) < share
    fast_rate = jax.random.uniform(fast_key, (HEADS,), jnp.float32, jnp.log(0.015), jnp.log(0.05))
    slow_rate = jax.random.uniform(slow_key, (HEADS,), jnp.float32, jnp.log(0.15), jnp.log(0.5)) - jnp.log(1.0 * TOKENS)
    return jnp.where(fast_pick, fast_rate, slow_rate)


def steps_of(own_key, shape, cuts, low, largest):
    loudness, own = 1.0, jax.random.fold_in(own_key, 6)
    for dim, parts in cuts:
        heights = jnp.exp(jax.random.uniform(jax.random.fold_in(own, dim), (parts,), jnp.float32, low / len(cuts), largest / len(cuts)))
        loudness = loudness * jnp.repeat(heights, shape[dim] // parts).reshape([-1 if axis == dim else 1 for axis in range(len(shape))])
    return loudness


def centred(key, dims, spread, most, split=(), kind=jnp.bfloat16):
    drawn = spread * jax.random.normal(key, dims, jnp.float32)
    if split:
        drawn = drawn * steps_of(key, dims, split, -0.22, 0.18)
    return jnp.clip(drawn, -most, most).astype(kind)


def setup_inputs(seed: int = 0) -> dict:
    streams_of = jax.random.split(jax.random.key(seed), 18)
    return {
        "arriving_hidden_sum": draw_arriving_hidden_sum(jax.random.fold_in(streams_of[17], 71), 0),
        "content_entries_clustered": centred(streams_of[1], (TOKENS, DI), 1.0, 6.0, ((0, 8), (1, 4))),
        "leaving_switch_entries": centred(streams_of[2], (TOKENS, DI), 1.0, 6.0, ((0, 8), (1, 4))),
        "linked_source_target_pairs": centred(streams_of[3], (TOKENS, GROUPS, 2, STATE), (STATE ** -0.25), 1.78125, ((0, 8), (1, 4))),
        "raw_interval_length": draw_raw_interval_length(jax.random.fold_in(streams_of[17], 71), 0),
        "spike_extra_lognoise": draw_spike_extra_lognoise(jax.random.fold_in(streams_of[17], 71), 0),
        "content_filter_kernel": centred(streams_of[6], (CONV, DI), CONV ** -0.5, 3.0, ((1, 4),)),
        "coupling_filter_kernel": centred(streams_of[7], (CONV, GROUPS, 2, STATE), CONV ** -0.5, 3.0, ((1, 4),)),
        "interval_shift_vector": jnp.clip(jax.random.uniform(streams_of[8], (HEADS,), jnp.float32, -0.5, 0.5) * steps_of(streams_of[8], (HEADS,), ((0, 4),), -0.4, 0.0), -0.5, 0.5),
        "fading_speed_exponent": draw_fading_speed_exponent(jax.random.fold_in(streams_of[17], 71), 0),
        "skip_channel_factor": jnp.clip(jnp.exp(math.log(10.0) - 2.3025851 * jax.random.uniform(streams_of[10], (HEADS,), jnp.float32) ** steps_of(streams_of[10], (HEADS,), ((0, 4),), -0.2, 0.2)), 1.0, 10.0),
        "cluster_rescale_vector": jnp.clip(1.0 + 0.18 * jax.random.normal(streams_of[11], (DI,), jnp.float32), 0.1, 1.9),
        "blender_final_tensor": centred(streams_of[12], (DI, D), DI ** -0.5, 0.09375, ((0, 4),)),
        "prelayer_rescale_vector": jnp.clip(1.0 + 0.18 * jax.random.normal(streams_of[13], (D,), jnp.float32), 0.1, 1.9),
        "switching_linear_tensor": centred(streams_of[14], (D, FF), D ** -0.5, 0.125, ((0, 8), (1, 4))),
        "widening_linear_tensor": centred(streams_of[15], (D, FF), D ** -0.5, 0.125, ((0, 8), (1, 4))),
        "contracting_linear_tensor": centred(streams_of[16], (FF, D), FF ** -0.5, 0.078125, ((0, 4), (1, 8))),
    }


EPS = 1e-06
highest = lax.Precision.HIGHEST

def causal_conv(values, taps):
    taps_count = taps.shape[0]
    length = values.shape[0]
    padded = jnp.pad(values.astype(jnp.float32), ((taps_count - 1, 0), (0, 0)))
    running = jnp.zeros(values.shape, jnp.float32)
    for tap_index in range(taps_count):
        running = running + padded[tap_index:tap_index + length] * taps[tap_index].astype(jnp.float32)
    return jax.nn.silu(running).astype(jnp.bfloat16)

def reference(arriving_hidden_sum, content_entries_clustered, leaving_switch_entries, linked_source_target_pairs, raw_interval_length, spike_extra_lognoise, content_filter_kernel, coupling_filter_kernel, interval_shift_vector, fading_speed_exponent, skip_channel_factor, cluster_rescale_vector, blender_final_tensor, prelayer_rescale_vector, switching_linear_tensor, widening_linear_tensor, contracting_linear_tensor):
    length = content_entries_clustered.shape[0]
    per_group = HEADS // GROUPS
    block_count = length // BLOCK_POSITIONS
    values = causal_conv(content_entries_clustered, content_filter_kernel)
    maps = causal_conv(linked_source_target_pairs.reshape(length, -1), coupling_filter_kernel.reshape(CONV, -1)).reshape(length, GROUPS, 2, STATE)
    write_map = maps[:, :, 0]
    read_map = maps[:, :, 1]
    interval_lengths = jax.nn.softplus(raw_interval_length.astype(jnp.float32) + interval_shift_vector)
    fading_log_factor = -jnp.exp(fading_speed_exponent) * interval_lengths + spike_extra_lognoise
    causal = jnp.tril(jnp.ones((BLOCK_POSITIONS, BLOCK_POSITIONS), bool))

    def block_step(carry_state, inputs):
        value_block, write_block, read_block, step_block, log_block = inputs
        cum_log = jnp.cumsum(log_block, axis=0)
        head_cum = cum_log.T
        log_gap = head_cum[:, :, None] - head_cum[:, None, :]
        intersection = jnp.einsum('lgn,sgn->gls', read_block.astype(jnp.float32), write_block.astype(jnp.float32))
        intersection = jnp.repeat(intersection, per_group, axis=0)
        weights = (intersection * jnp.exp(jnp.where(causal, log_gap, -jnp.inf)) * step_block.T[:, None, :]).astype(jnp.bfloat16)
        within = jnp.einsum('hls,shp->lhp', weights.astype(jnp.float32), value_block.astype(jnp.float32))
        carried = jnp.einsum('lgn,grpn->lgrp', read_block.astype(jnp.float32), carry_state, precision=highest)
        carried = carried.reshape(BLOCK_POSITIONS, HEADS, HEAD_DIM) * jnp.exp(cum_log)[:, :, None]
        end_log = cum_log[-1]
        scaled = (value_block.astype(jnp.float32) * (step_block * jnp.exp(end_log[None, :] - cum_log))[:, :, None]).astype(jnp.bfloat16)
        block_states = jnp.einsum('lgn,lgrp->grpn', write_block.astype(jnp.float32), scaled.astype(jnp.float32).reshape(BLOCK_POSITIONS, GROUPS, per_group, HEAD_DIM))
        carry_state = carry_state * jnp.exp(end_log).reshape(GROUPS, per_group)[:, :, None, None] + block_states
        return (carry_state, within + carried)
    value_heads = values.reshape(length, HEADS, HEAD_DIM)
    inputs = (value_heads.reshape(block_count, BLOCK_POSITIONS, HEADS, HEAD_DIM), write_map.reshape(block_count, BLOCK_POSITIONS, GROUPS, STATE), read_map.reshape(block_count, BLOCK_POSITIONS, GROUPS, STATE), interval_lengths.reshape(block_count, BLOCK_POSITIONS, HEADS), fading_log_factor.reshape(block_count, BLOCK_POSITIONS, HEADS))
    start_state = jnp.zeros((GROUPS, per_group, HEAD_DIM, STATE), jnp.float32)
    _, mixer = lax.scan(block_step, start_state, inputs)
    mixer = mixer.reshape(length, HEADS, HEAD_DIM) + value_heads.astype(jnp.float32) * skip_channel_factor[None, :, None]
    gated = mixer.reshape(length, DI) * jax.nn.silu(leaving_switch_entries.astype(jnp.float32))
    grouped = gated.reshape(length, GROUPS, DI // GROUPS)
    grouped = grouped * lax.rsqrt(lax.optimization_barrier(jnp.mean(grouped * grouped, axis=-1, keepdims=True)) + EPS)
    mixed_rows = (grouped.reshape(length, DI) * cluster_rescale_vector).astype(jnp.bfloat16)
    part_width = DI // N_TP
    mixer_out = jnp.zeros((length, D), jnp.float32)
    for device_rank in range(N_TP):
        partial_sum = jnp.dot(mixed_rows[:, device_rank * part_width:(device_rank + 1) * part_width], blender_final_tensor[device_rank * part_width:(device_rank + 1) * part_width], preferred_element_type=jnp.float32)
        mixer_out = mixer_out + lax.optimization_barrier(partial_sum.astype(jnp.bfloat16)).astype(jnp.float32)
    residual_mid = (arriving_hidden_sum.astype(jnp.float32) + mixer_out).astype(jnp.bfloat16)
    squares = residual_mid.astype(jnp.float32)
    normed = (squares * lax.rsqrt(lax.optimization_barrier(jnp.mean(squares * squares, axis=-1, keepdims=True)) + EPS) * prelayer_rescale_vector).astype(jnp.bfloat16)
    gate_pre = jnp.dot(normed, switching_linear_tensor, preferred_element_type=jnp.float32)
    up_pre = jnp.dot(normed, widening_linear_tensor, preferred_element_type=jnp.float32)
    hidden = (jax.nn.silu(gate_pre) * up_pre).astype(jnp.bfloat16)
    hidden_width = FF // N_TP
    mlp_out = jnp.zeros((length, D), jnp.float32)
    for device_rank in range(N_TP):
        partial_sum = jnp.dot(hidden[:, device_rank * hidden_width:(device_rank + 1) * hidden_width], contracting_linear_tensor[device_rank * hidden_width:(device_rank + 1) * hidden_width], preferred_element_type=jnp.float32)
        mlp_out = mlp_out + lax.optimization_barrier(partial_sum.astype(jnp.bfloat16)).astype(jnp.float32)
    return (residual_mid.astype(jnp.float32) + 0.5 * mlp_out).astype(jnp.bfloat16)
```

```python
import jax
import jax.numpy as jnp
from jax import lax
from jax.sharding import PartitionSpec as P

D = 2048
BLOCK_POSITIONS = 128


EPS = 1e-06
highest = lax.Precision.HIGHEST


def from_behind(block, axis, distance):
    devices = range(lax.axis_size(axis))
    route = [(i - distance, i) for i in devices if i - distance in devices]
    return lax.ppermute(block, axis, route)


def ring_order(count):
    inner = 1
    while inner * inner * 4 <= count:
        inner *= 2
    outer = count // inner
    if inner == 1 or outer % 2:
        return list(range(count))
    order = [z * inner for z in range(outer)]
    for lap, z in enumerate(reversed(range(outer))):
        ys = range(1, inner) if lap % 2 == 0 else range(inner - 1, 0, -1)
        order += [z * inner + y for y in ys]
    return order


def ring_places(axis):
    count = lax.axis_size(axis)
    order = ring_order(count)
    up = [(order[i], order[(i + 1) % count]) for i in range(count)]
    down = [(b, a) for a, b in up]
    place = jnp.asarray([order.index(i) for i in range(count)], jnp.int32)[lax.axis_index(axis)]
    return up, down, place, jnp.asarray(order, jnp.int32)


def ring_hops(fronts, axis, hop):
    count = lax.axis_size(axis)
    up, down, _, _ = ring_places(axis)
    moved = []
    for index, (ahead, behind) in enumerate(fronts):
        last = 2 * hop == count
        both = 2 * hop < count
        if both or (last and index % 2 == 0):
            ahead = lax.ppermute(ahead, axis, up)
        if both or (last and index % 2 == 1):
            behind = lax.ppermute(behind, axis, down)
        moved.append((ahead, behind))
    return moved


def ring_whole(index, own, history, axis):
    count = lax.axis_size(axis)
    _, _, place, owners = ring_places(axis)
    parts = [(own, 0)]
    for hop, fronts in enumerate(history, 1):
        last, both = 2 * hop == count, 2 * hop < count
        if both or (last and index % 2 == 0):
            parts.append((fronts[index][0], -hop))
        if both or (last and index % 2 == 1):
            parts.append((fronts[index][1], hop))
    whole = jnp.zeros((count,) + own.shape, own.dtype)
    for part, shift in parts:
        owner = owners[(place + shift) % count]
        whole = lax.dynamic_update_index_in_dim(whole, part, owner, 0)
    return whole


def conv_block(values, rims, taps):
    taps_count = taps.shape[0]
    length = values.shape[0]
    padded = jnp.concatenate([rims, values], axis=0).astype(jnp.float32)
    running = jnp.zeros(values.shape, jnp.float32)
    for tap_index in range(taps_count):
        running = running + padded[tap_index : tap_index + length] * taps[tap_index].astype(
            jnp.float32
        )
    return jax.nn.silu(running).astype(jnp.bfloat16)


def shards(
    arriving_hidden_sum,
    content_entries_clustered,
    leaving_switch_entries,
    linked_source_target_pairs,
    raw_interval_length,
    spike_extra_lognoise,
    content_filter_kernel,
    coupling_filter_kernel,
    interval_shift_vector,
    fading_speed_exponent,
    skip_channel_factor,
    cluster_rescale_vector,
    blender_final_tensor,
    prelayer_rescale_vector,
    switching_linear_tensor,
    widening_linear_tensor,
    contracting_linear_tensor,
):
    length = content_entries_clustered.shape[0]
    heads_per_device = raw_interval_length.shape[1]
    groups_dev = linked_source_target_pairs.shape[1]
    per_group = heads_per_device // groups_dev
    head_size = content_entries_clustered.shape[1] // heads_per_device
    state_size = linked_source_target_pairs.shape[3]
    taps_count = content_filter_kernel.shape[0]
    block_count = length // BLOCK_POSITIONS
    couple_flat = linked_source_target_pairs.reshape(length, -1)
    value_rims, couple_rims = from_behind(
        (
            content_entries_clustered[length - taps_count + 1 :],
            couple_flat[length - taps_count + 1 :],
        ),
        "sp",
        1,
    )
    owned = (switching_linear_tensor, widening_linear_tensor, contracting_linear_tensor)
    value_rims, couple_rims, owned = lax.optimization_barrier((value_rims, couple_rims, owned))
    hops = lax.axis_size("sp") // 2
    history = [ring_hops([(part, part) for part in owned], "sp", 1)]
    values = conv_block(content_entries_clustered, value_rims, content_filter_kernel)
    coupled = conv_block(
        couple_flat, couple_rims, coupling_filter_kernel.reshape(taps_count, -1)
    ).reshape(length, groups_dev, 2, state_size)
    (values, coupled), history[0] = lax.optimization_barrier(((values, coupled), history[0]))
    for hop in range(2, hops // 2 + 1):
        history.append(ring_hops(history[-1], "sp", hop))
    value_blocks = values.reshape(block_count, BLOCK_POSITIONS, heads_per_device, head_size)
    write_maps = coupled[:, :, 0].reshape(block_count, BLOCK_POSITIONS, groups_dev, state_size)
    read_maps = coupled[:, :, 1].reshape(block_count, BLOCK_POSITIONS, groups_dev, state_size)
    interval_lengths = jax.nn.softplus(
        raw_interval_length.astype(jnp.float32) + interval_shift_vector
    )
    fading_log_factor = (
        -jnp.exp(fading_speed_exponent) * interval_lengths + spike_extra_lognoise
    ).reshape(block_count, BLOCK_POSITIONS, heads_per_device)
    interval_lengths = interval_lengths.reshape(block_count, BLOCK_POSITIONS, heads_per_device)
    causal = jnp.tril(jnp.ones((BLOCK_POSITIONS, BLOCK_POSITIONS), bool))
    cum_log = jnp.einsum(
        "ts,bsh->bth", causal.astype(jnp.float32), fading_log_factor, precision=highest
    )
    head_cum = jnp.swapaxes(cum_log, 1, 2)
    log_gap = head_cum[:, :, :, None] - head_cum[:, :, None, :]
    intersection = jnp.einsum(
        "blgn,bsgn->bgls", read_maps, write_maps, preferred_element_type=jnp.float32
    )
    intersection = jnp.repeat(intersection, per_group, axis=1)
    weights = (
        intersection
        * jnp.exp(jnp.where(causal, log_gap, -jnp.inf))
        * jnp.swapaxes(interval_lengths, 1, 2)[:, :, None, :]
    ).astype(jnp.bfloat16)
    within = jnp.einsum(
        "bhls,bshp->blhp", weights, value_blocks, preferred_element_type=jnp.float32
    )
    end_log = cum_log[:, -1]
    scaled = (
        value_blocks * (interval_lengths * jnp.exp(end_log[:, None, :] - cum_log))[..., None]
    ).astype(jnp.bfloat16)
    block_states = jnp.einsum(
        "blgn,blgrp->bgrpn",
        write_maps,
        scaled.reshape(block_count, BLOCK_POSITIONS, groups_dev, per_group, head_size),
        preferred_element_type=jnp.float32,
    )
    end_grouped = end_log.reshape(block_count, groups_dev, per_group)
    carry_state = jnp.zeros((groups_dev, per_group, head_size, state_size), jnp.float32)
    entering = []
    for block in range(block_count):
        entering.append(carry_state)
        decay = jnp.exp(end_grouped[block])[:, :, None, None]
        carry_state = carry_state * decay + block_states[block]
    device_log = jnp.sum(end_log, axis=0)
    log_rows = -(-heads_per_device // 16) * 16
    message = jnp.concatenate(
        [
            carry_state.reshape(-1, state_size),
            jnp.broadcast_to(
                jnp.pad(device_log, (0, log_rows - heads_per_device))[:, None],
                (log_rows, state_size),
            ),
        ],
        axis=0,
    ).astype(jnp.bfloat16)
    everyone = lax.all_gather(message, "sp")
    state_rows = heads_per_device * head_size
    their_logs = everyone[:, state_rows : state_rows + heads_per_device, 0].astype(jnp.float32)
    sp_count, sp_place = lax.axis_size("sp"), lax.axis_index("sp")
    ranks = jnp.arange(sp_count)
    counted = (ranks < sp_place)[:, None]
    kept_logs = jnp.where(counted, their_logs, 0.0)
    later_logs = jnp.sum(kept_logs, axis=0) - jnp.cumsum(kept_logs, axis=0)
    factors = jnp.where(counted, jnp.exp(later_logs), 0.0).reshape(
        sp_count, groups_dev, per_group, 1, 1
    )
    incoming = jnp.sum(
        everyone[:, :state_rows]
        .reshape(sp_count, groups_dev, per_group, head_size, state_size)
        .astype(jnp.float32)
        * factors,
        axis=0,
    )
    prior_log = jnp.cumsum(end_log, axis=0) - end_log
    prior_grouped = prior_log.reshape(block_count, groups_dev, per_group)
    states = jnp.stack(entering) + jnp.exp(prior_grouped)[..., None, None] * incoming
    carried = (
        jnp.einsum(
            "blgn,bgrpn->blgrp",
            read_maps,
            states.astype(jnp.bfloat16),
            preferred_element_type=jnp.float32,
        ).reshape(block_count, BLOCK_POSITIONS, heads_per_device, head_size)
        * jnp.exp(cum_log)[..., None]
    )
    mixer = (within + carried).reshape(
        length, heads_per_device, head_size
    ) + values.reshape(length, heads_per_device, head_size).astype(
        jnp.float32
    ) * skip_channel_factor[
        None, :, None
    ]
    early = hops // 2
    mixer, history[early - 1] = lax.optimization_barrier((mixer, history[early - 1]))
    for hop in range(early + 1, hops + 1):
        history.append(ring_hops(history[hop - 2], "sp", hop))
    gated = mixer.reshape(length, heads_per_device * head_size) * jax.nn.silu(
        leaving_switch_entries.astype(jnp.float32)
    )
    grouped = gated.reshape(length, groups_dev, per_group * head_size)
    grouped = grouped * lax.rsqrt(jnp.mean(grouped * grouped, axis=-1, keepdims=True) + EPS)
    mixed_rows = (
        grouped.reshape(length, heads_per_device * head_size) * cluster_rescale_vector
    ).astype(jnp.bfloat16)
    partial_sum = jnp.dot(mixed_rows, blender_final_tensor, preferred_element_type=jnp.float32)
    rounded = lax.optimization_barrier(partial_sum.astype(jnp.bfloat16)).astype(jnp.float32)
    col_count = D // lax.axis_size("tp")
    offset = lax.axis_index("tp") * col_count
    mixer_cols = lax.psum_scatter(
        rounded.astype(jnp.bfloat16), "tp", scatter_dimension=1, tiled=True
    ).astype(jnp.float32)
    resid_cols = lax.dynamic_slice_in_dim(arriving_hidden_sum, offset, col_count, 1)
    residual_mid = (resid_cols.astype(jnp.float32) + mixer_cols).astype(jnp.bfloat16)
    squares = residual_mid.astype(jnp.float32)
    square_sums = lax.psum(jnp.sum(squares * squares, axis=1), "tp")
    gain_cols = lax.dynamic_slice_in_dim(prelayer_rescale_vector, offset, col_count, 0)
    normed_cols = (squares * lax.rsqrt(square_sums / D + EPS)[:, None] * gain_cols).astype(
        jnp.bfloat16
    )
    normed = lax.all_gather(normed_cols, "tp", axis=1, tiled=True)
    gate_whole, up_whole, down_whole = (
        ring_whole(index, part, history, "sp") for index, part in enumerate(owned)
    )
    gate_whole = gate_whole.reshape(-1, gate_whole.shape[2])
    up_whole = up_whole.reshape(-1, up_whole.shape[2])
    down_whole = jnp.swapaxes(down_whole, 0, 1).reshape(down_whole.shape[1], -1)
    gate_pre = jnp.dot(
        normed,
        gate_whole,
        preferred_element_type=jnp.float32,
    )
    up_pre = jnp.dot(
        normed,
        up_whole,
        preferred_element_type=jnp.float32,
    )
    hidden = (jax.nn.silu(gate_pre) * up_pre).astype(jnp.bfloat16)
    down_terms = jnp.dot(
        hidden,
        down_whole,
        preferred_element_type=jnp.float32,
    )
    down_rounded = lax.optimization_barrier(down_terms.astype(jnp.bfloat16)).astype(jnp.float32)
    mlp_cols = lax.psum_scatter(
        down_rounded.astype(jnp.bfloat16), "tp", scatter_dimension=1, tiled=True
    ).astype(jnp.float32)
    return (residual_mid.astype(jnp.float32) + 0.5 * mlp_cols).astype(jnp.bfloat16)


def solution(mesh):
    placed = (
        P("sp", None),
        P("sp", "tp"),
        P("sp", "tp"),
        P("sp", "tp", None, None),
        P("sp", "tp"),
        P("sp", "tp"),
        P(None, "tp"),
        P(None, "tp", None, None),
        P("tp"),
        P("tp"),
        P("tp"),
        P("tp"),
        P("tp", None),
        P(),
        P("sp", "tp"),
        P("sp", "tp"),
        P("tp", "sp"),
    )
    return jax.shard_map(
        shards, mesh=mesh, in_specs=placed, out_specs=P("sp", "tp"), check_vma=False
    )
```

```python
import jax
import jax.numpy as jnp
from jax import lax
from jax.sharding import PartitionSpec as P

D = 2048
BLOCK_POSITIONS = 128


EPS = 1e-06
highest = lax.Precision.HIGHEST


def from_behind(block, axis, distance):
    devices = range(lax.axis_size(axis))
    route = [(i - distance, i) for i in devices if i - distance in devices]
    return lax.ppermute(block, axis, route)


def ring_order(count):
    inner = 1
    while inner * inner * 4 <= count:
        inner *= 2
    outer = count // inner
    if inner == 1 or outer % 2:
        return list(range(count))
    order = [z * inner for z in range(outer)]
    for lap, z in enumerate(reversed(range(outer))):
        ys = range(1, inner) if lap % 2 == 0 else range(inner - 1, 0, -1)
        order += [z * inner + y for y in ys]
    return order


def ring_places(axis):
    count = lax.axis_size(axis)
    order = ring_order(count)
    up = [(order[i], order[(i + 1) % count]) for i in range(count)]
    down = [(b, a) for a, b in up]
    place = jnp.asarray([order.index(i) for i in range(count)], jnp.int32)[lax.axis_index(axis)]
    return up, down, place, jnp.asarray(order, jnp.int32)


def ring_hops(fronts, axis, hop):
    count = lax.axis_size(axis)
    up, down, _, _ = ring_places(axis)
    moved = []
    for index, (ahead, behind) in enumerate(fronts):
        last = 2 * hop == count
        both = 2 * hop < count
        if both or (last and index % 2 == 0):
            ahead = lax.ppermute(ahead, axis, up)
        if both or (last and index % 2 == 1):
            behind = lax.ppermute(behind, axis, down)
        moved.append((ahead, behind))
    return moved


def ring_whole(index, own, history, axis):
    count = lax.axis_size(axis)
    _, _, place, owners = ring_places(axis)
    parts = [(own, 0)]
    for hop, fronts in enumerate(history, 1):
        last, both = 2 * hop == count, 2 * hop < count
        if both or (last and index % 2 == 0):
            parts.append((fronts[index][0], -hop))
        if both or (last and index % 2 == 1):
            parts.append((fronts[index][1], hop))
    whole = jnp.zeros((count,) + own.shape, own.dtype)
    for part, shift in parts:
        owner = owners[(place + shift) % count]
        whole = lax.dynamic_update_index_in_dim(whole, part, owner, 0)
    return whole


def conv_block(values, rims, taps):
    taps_count = taps.shape[0]
    length = values.shape[0]
    padded = jnp.concatenate([rims, values], axis=0).astype(jnp.float32)
    running = jnp.zeros(values.shape, jnp.float32)
    for tap_index in range(taps_count):
        running = running + padded[tap_index : tap_index + length] * taps[tap_index].astype(
            jnp.float32
        )
    return jax.nn.silu(running).astype(jnp.bfloat16)


def shards(
    arriving_hidden_sum,
    content_entries_clustered,
    leaving_switch_entries,
    linked_source_target_pairs,
    raw_interval_length,
    spike_extra_lognoise,
    content_filter_kernel,
    coupling_filter_kernel,
    interval_shift_vector,
    fading_speed_exponent,
    skip_channel_factor,
    cluster_rescale_vector,
    blender_final_tensor,
    prelayer_rescale_vector,
    switching_linear_tensor,
    widening_linear_tensor,
    contracting_linear_tensor,
):
    length = content_entries_clustered.shape[0]
    heads_per_device = raw_interval_length.shape[1]
    groups_dev = linked_source_target_pairs.shape[1]
    per_group = heads_per_device // groups_dev
    head_size = content_entries_clustered.shape[1] // heads_per_device
    state_size = linked_source_target_pairs.shape[3]
    taps_count = content_filter_kernel.shape[0]
    block_count = length // BLOCK_POSITIONS
    couple_flat = linked_source_target_pairs.reshape(length, -1)
    value_rims, couple_rims = from_behind(
        (
            content_entries_clustered[length - taps_count + 1 :],
            couple_flat[length - taps_count + 1 :],
        ),
        "sp",
        1,
    )
    owned = (switching_linear_tensor, widening_linear_tensor, contracting_linear_tensor)
    (
        value_rims,
        couple_rims,
        owned,
        content_entries_clustered,
        couple_flat,
        raw_interval_length,
    ) = lax.optimization_barrier(
        (
            value_rims,
            couple_rims,
            owned,
            content_entries_clustered,
            couple_flat,
            raw_interval_length,
        )
    )
    hops = lax.axis_size("sp") // 2
    history = [ring_hops([(part, part) for part in owned], "sp", 1)]
    values = conv_block(content_entries_clustered, value_rims, content_filter_kernel)
    coupled = conv_block(
        couple_flat, couple_rims, coupling_filter_kernel.reshape(taps_count, -1)
    ).reshape(length, groups_dev, 2, state_size)
    (values, coupled), history[0] = lax.optimization_barrier(((values, coupled), history[0]))
    for hop in range(2, hops // 2 + 1):
        history.append(ring_hops(history[-1], "sp", hop))
    value_blocks = values.reshape(block_count, BLOCK_POSITIONS, heads_per_device, head_size)
    write_maps = coupled[:, :, 0].reshape(block_count, BLOCK_POSITIONS, groups_dev, state_size)
    read_maps = coupled[:, :, 1].reshape(block_count, BLOCK_POSITIONS, groups_dev, state_size)
    interval_lengths = jax.nn.softplus(
        raw_interval_length.astype(jnp.float32) + interval_shift_vector
    )
    fading_log_factor = (
        -jnp.exp(fading_speed_exponent) * interval_lengths + spike_extra_lognoise
    ).reshape(block_count, BLOCK_POSITIONS, heads_per_device)
    interval_lengths = interval_lengths.reshape(block_count, BLOCK_POSITIONS, heads_per_device)
    causal = jnp.tril(jnp.ones((BLOCK_POSITIONS, BLOCK_POSITIONS), bool))
    cum_log = jnp.einsum(
        "ts,bsh->bth", causal.astype(jnp.float32), fading_log_factor, precision=highest
    )
    head_cum = jnp.swapaxes(cum_log, 1, 2)
    log_gap = head_cum[:, :, :, None] - head_cum[:, :, None, :]
    intersection = jnp.einsum(
        "blgn,bsgn->bgls", read_maps, write_maps, preferred_element_type=jnp.float32
    )
    intersection = jnp.repeat(intersection, per_group, axis=1)
    weights = (
        intersection
        * jnp.exp(jnp.where(causal, log_gap, -jnp.inf))
        * jnp.swapaxes(interval_lengths, 1, 2)[:, :, None, :]
    ).astype(jnp.bfloat16)
    within = jnp.einsum(
        "bhls,bshp->blhp", weights, value_blocks, preferred_element_type=jnp.float32
    )
    end_log = cum_log[:, -1]
    scaled = (
        value_blocks * (interval_lengths * jnp.exp(end_log[:, None, :] - cum_log))[..., None]
    ).astype(jnp.bfloat16)
    block_states = jnp.einsum(
        "blgn,blgrp->bgrpn",
        write_maps,
        scaled.reshape(block_count, BLOCK_POSITIONS, groups_dev, per_group, head_size),
        preferred_element_type=jnp.float32,
    )
    end_grouped = end_log.reshape(block_count, groups_dev, per_group)
    carry_state = jnp.zeros((groups_dev, per_group, head_size, state_size), jnp.float32)
    entering = []
    end_decays = lax.optimization_barrier(
        jnp.broadcast_to(jnp.exp(end_grouped)[..., None], end_grouped.shape + (state_size,))
    )
    for block in range(block_count):
        entering.append(carry_state)
        decay = end_decays[block][:, :, None, :]
        carry_state = carry_state * decay + block_states[block]
    device_log = jnp.sum(end_log, axis=0)
    log_rows = -(-heads_per_device // 16) * 16
    message = jnp.concatenate(
        [
            carry_state.reshape(-1, state_size),
            jnp.broadcast_to(
                jnp.pad(device_log, (0, log_rows - heads_per_device))[:, None],
                (log_rows, state_size),
            ),
        ],
        axis=0,
    ).astype(jnp.bfloat16)
    everyone = lax.all_gather(message, "sp")
    state_rows = heads_per_device * head_size
    their_logs = everyone[:, state_rows : state_rows + heads_per_device, 0].astype(jnp.float32)
    sp_count, sp_place = lax.axis_size("sp"), lax.axis_index("sp")
    ranks = jnp.arange(sp_count)
    counted = (ranks < sp_place)[:, None]
    kept_logs = jnp.where(counted, their_logs, 0.0)
    later_logs = jnp.sum(kept_logs, axis=0) - jnp.cumsum(kept_logs, axis=0)
    factors = jnp.where(counted, jnp.exp(later_logs), 0.0).reshape(
        sp_count, groups_dev, per_group, 1, 1
    )
    incoming = jnp.sum(
        everyone[:, :state_rows]
        .reshape(sp_count, groups_dev, per_group, head_size, state_size)
        .astype(jnp.float32)
        * factors,
        axis=0,
    )
    prior_log = jnp.cumsum(end_log, axis=0) - end_log
    prior_grouped = prior_log.reshape(block_count, groups_dev, per_group)
    states = jnp.stack(entering) + jnp.exp(prior_grouped)[..., None, None] * incoming
    carried = (
        jnp.einsum(
            "blgn,bgrpn->blgrp",
            read_maps,
            states.astype(jnp.bfloat16),
            preferred_element_type=jnp.float32,
        ).reshape(block_count, BLOCK_POSITIONS, heads_per_device, head_size)
        * jnp.exp(cum_log)[..., None]
    )
    mixer = (within + carried).reshape(
        length, heads_per_device, head_size
    ) + values.reshape(length, heads_per_device, head_size).astype(
        jnp.float32
    ) * skip_channel_factor[
        None, :, None
    ]
    early = hops // 2
    mixer, history[early - 1] = lax.optimization_barrier((mixer, history[early - 1]))
    third = early + (hops - early + 1) // 2
    for hop in range(early + 1, third + 1):
        history.append(ring_hops(history[hop - 2], "sp", hop))
    gated = mixer.reshape(length, heads_per_device * head_size) * jax.nn.silu(
        leaving_switch_entries.astype(jnp.float32)
    )
    grouped = gated.reshape(length, groups_dev, per_group * head_size)
    grouped = grouped * lax.rsqrt(jnp.mean(grouped * grouped, axis=-1, keepdims=True) + EPS)
    mixed_rows = (
        grouped.reshape(length, heads_per_device * head_size) * cluster_rescale_vector
    ).astype(jnp.bfloat16)
    partial_sum = jnp.dot(mixed_rows, blender_final_tensor, preferred_element_type=jnp.float32)
    rounded = lax.optimization_barrier(partial_sum.astype(jnp.bfloat16)).astype(jnp.float32)
    col_count = D // lax.axis_size("tp")
    offset = lax.axis_index("tp") * col_count
    mixer_cols = lax.psum_scatter(
        rounded.astype(jnp.bfloat16), "tp", scatter_dimension=1, tiled=True
    ).astype(jnp.float32)
    mixer_cols, history, owned = lax.optimization_barrier((mixer_cols, history, owned))
    for hop in range(third + 1, hops + 1):
        history.append(ring_hops(history[-1], "sp", hop))
    resid_cols = lax.dynamic_slice_in_dim(arriving_hidden_sum, offset, col_count, 1)
    residual_mid = (resid_cols.astype(jnp.float32) + mixer_cols).astype(jnp.bfloat16)
    squares = residual_mid.astype(jnp.float32)
    square_sums = lax.psum(jnp.sum(squares * squares, axis=1), "tp")
    gain_cols = lax.dynamic_slice_in_dim(prelayer_rescale_vector, offset, col_count, 0)
    normed_cols = (squares * lax.rsqrt(square_sums / D + EPS)[:, None] * gain_cols).astype(
        jnp.bfloat16
    )
    normed = lax.all_gather(normed_cols, "tp", axis=1, tiled=True)
    gate_whole, up_whole, down_whole = (
        ring_whole(index, part, history, "sp") for index, part in enumerate(owned)
    )
    gate_whole = gate_whole.reshape(-1, gate_whole.shape[2])
    up_whole = up_whole.reshape(-1, up_whole.shape[2])
    down_whole = jnp.swapaxes(down_whole, 0, 1).reshape(down_whole.shape[1], -1)
    gate_pre = jnp.dot(
        normed,
        gate_whole,
        preferred_element_type=jnp.float32,
    )
    up_pre = jnp.dot(
        normed,
        up_whole,
        preferred_element_type=jnp.float32,
    )
    hidden = (jax.nn.silu(gate_pre) * up_pre).astype(jnp.bfloat16)
    down_terms = jnp.dot(
        hidden,
        down_whole,
        preferred_element_type=jnp.float32,
    )
    down_rounded = lax.optimization_barrier(down_terms.astype(jnp.bfloat16)).astype(jnp.float32)
    mlp_cols = lax.psum_scatter(
        down_rounded.astype(jnp.bfloat16), "tp", scatter_dimension=1, tiled=True
    ).astype(jnp.float32)
    return (residual_mid.astype(jnp.float32) + 0.5 * mlp_cols).astype(jnp.bfloat16)


def solution(mesh):
    placed = (
        P("sp", None),
        P("sp", "tp"),
        P("sp", "tp"),
        P("sp", "tp", None, None),
        P("sp", "tp"),
        P("sp", "tp"),
        P(None, "tp"),
        P(None, "tp", None, None),
        P("tp"),
        P("tp"),
        P("tp"),
        P("tp"),
        P("tp", None),
        P(),
        P("sp", "tp"),
        P("sp", "tp"),
        P("tp", "sp"),
    )
    return jax.shard_map(
        shards, mesh=mesh, in_specs=placed, out_specs=P("sp", "tp"), check_vma=False
    )
```
